32 devices in a mesh: grp: 2 (over y), ep: 4 (over z), tp: 4 (over x, core).
Axes of the slice: x: 2, y: 2, z: 4, core: 2. Of those that a mesh axis runs over, the one named last changes fastest.
Arguments:
- tokens: bfloat16 [8, 2048], P(('grp', 'ep')), parts along dimension 0, may hold values from -6 to 6
- conv_state: bfloat16 [8, 3, 1024], P(('grp', 'ep'), None, 'tp'), parts along dimension 0, may hold values from -6 to 6
- state_h: float32 [8, 1024], P(('grp', 'ep'), 'tp'), parts along dimension 0, may hold values from -6 to 6
- mixer_gain: bfloat16 [2048], replicated, may hold values from 0.099609375 to 1.8984375
- expert_gain: bfloat16 [2048], replicated, may hold values from 0.099609375 to 1.8984375
- input_proj: bfloat16 [2048, 1024], P('ep', 'tp'), may hold values from -0.125 to 0.125
- branch_proj: bfloat16 [2048, 1024], P('ep', 'tp'), may hold values from -0.125 to 0.125
- conv_taps: bfloat16 [4, 1024], P(None, 'tp'), may hold values from -3 to 3
- write_map: bfloat16 [8, 128, 128], P('tp'), may hold values from -0.5 to 0.5
- decay_map: bfloat16 [8, 128, 128], P('tp'), may hold values from -0.5 to 0.5
- decay_rate: float32 [1024], P('tp'), may hold values from 0.01 to 0.4
- output_proj: bfloat16 [1024, 2048], P('tp'), may hold values from -0.1875 to 0.1875
- route_ids: int32 [8, 2], P('grp'), parts along dimension 0, may hold values from 0 to 3, all different within a row; in each aligned block of 4 rows (0 to 3, 4 to 7, ...) at most 4 rows name the same one
- route_scores: float32 [8, 2], P('grp'), parts along dimension 0, may hold values from 0.5 to 4
- expert_gate: bfloat16 [4, 2048, 1024], P('ep', None, 'tp'), may hold values from -0.125 to 0.125
- expert_up: bfloat16 [4, 2048, 1024], P('ep', None, 'tp'), may hold values from -0.125 to 0.125
- expert_down: bfloat16 [4, 1024, 2048], P('ep', 'tp'), may hold values from -0.1875 to 0.1875
- branch_gate: bfloat16 [2048], replicated, may hold values from -0.125 to 0.125
- shared_gate: bfloat16 [2048, 16384], P(None, ('ep', 'tp')), may hold values from -0.125 to 0.125
- shared_up: bfloat16 [2048, 16384], P(None, ('ep', 'tp')), may hold values from -0.125 to 0.125
- shared_down: bfloat16 [16384, 2048], P(('ep', 'tp')), may hold values from -0.0625 to 0.0625
Outputs:
- result: bfloat16 [8, 2048], P(('grp', 'ep'), 'tp'), parts along dimension 0
- state_next: float32 [8, 1024], P(('grp', 'ep'), 'tp'), parts along dimension 0
- conv_next: bfloat16 [8, 3, 1024], P(('grp', 'ep'), None, 'tp'), parts along dimension 0
The draws below stay inside these ranges and needn't reach their ends.
There are 2 independent parts, one for each index of `grp`. The reference program is written for one: setup_inputs(seed, part) draws one part's arguments, and reference() takes and returns one part's arrays. A program takes and returns all parts, laid end to end along the dimension named above; an argument that names none is the same for every part. Nothing has to cross between parts.
Inputs may be any that keep to these rules, and one draw needn't show every extreme that they name: `route_ids`: the 2 experts of a token differ; no expert is named by more than 4 tokens, a bound that some block reaches.
All inputs are finite; a program needn't handle non-finite values.
Results may differ from the reference program's by a relative error of at most 0.013.
Values may be sent and summed in bfloat16 or wider, within the bound.
A program may use at most 64 MiB of HBM per device.

```python
import math
import jax
import jax.numpy as jnp
import numpy as np
from jax import lax

D = 2048
LRU_HEADS = 8
HEAD_W = 128
CONV_W = 4
EXP_FF = 1024
DENSE_FF = 16384
TOPK = 2
LRU = 1024
TOKENS = 4
EXPERTS = 4
CAP = 4


def raised(values, key, source, target, blocks, factor):
    def block_of(axis_at):
        return (jnp.arange(values.shape[axis_at]) // (values.shape[axis_at] // blocks)).reshape((-1,) + (1,) * (values.ndim - 1 - axis_at))

    one_side = jax.random.permutation(key, blocks)[block_of(target)]
    second = (block_of(target) + blocks // 2) % blocks
    return jnp.where((block_of(source) == one_side) | (block_of(source) == second), factor * values, values)


def block_scale(key, extent, split, least, high):
    factor_of = 1.0
    for dim, shards_of in split:
        steps = jax.random.uniform(jax.random.fold_in(jax.random.fold_in(key, 6), dim), (shards_of,), jnp.float32, least / len(split), high / len(split))
        factor_of = factor_of * jnp.repeat(jnp.exp(steps), extent[dim] // shards_of).reshape((-1,) + (1,) * (len(extent) - 1 - dim))
    return factor_of


def routed_block(stream_key, own, number, rows, number_of, top, bound, lean):
    ranking = jax.random.permutation(stream_key, number_of)
    crowded, common = shares(number_of, rows * top, bound, lean, True), shares(number_of, rows * top, bound, lean, False)
    places = jnp.arange(number_of)

    def named(tallies, offset_by):
        used = int((tallies > 0).sum())
        fixed = max(1, used // 4)
        passed = fixed + (places - fixed + offset_by * (used - fixed)) % max(1, number_of - fixed)
        return jnp.zeros((number_of,), jnp.int32).at[ranking[jnp.where(places < fixed, places, passed)]].set(jnp.asarray(tallies, jnp.int32))

    tallies = jnp.where(number % 4 == 0, named(crowded, number // 4), named(common, number - number // 4 - 1))
    mixed = jax.random.permutation(jax.random.fold_in(own, 3), number_of)
    donor, receiver = mixed[0:number_of // 2 * 2:2], mixed[1:number_of // 2 * 2:2]
    margin = jnp.minimum(tallies[donor] - 1, bound - tallies[receiver]) // 2
    margin = jnp.where((donor == ranking[0]) | (receiver == ranking[0]) | (tallies[receiver] == 0), 0, jnp.maximum(margin, 0))
    passed = jax.random.randint(jax.random.fold_in(own, 4), (number_of // 2,), 0, 1 << 20) % (margin + 1)
    tallies = tallies.at[donor].add(-passed).at[receiver].add(passed)
    labels = jnp.searchsorted(jnp.cumsum(tallies), jnp.arange(rows * top), side="right").astype(jnp.int32)
    grid = labels.reshape(top, rows).T
    grid = grid[jax.random.permutation(jax.random.fold_in(own, 1), rows)]
    offset_by = jax.random.randint(jax.random.fold_in(own, 2), (rows, 1), 0, top)
    return jnp.take_along_axis(grid, (jnp.arange(top)[None, :] + offset_by) % top, axis=1)


def shares(count, total, reach, slope, full):
    weights = [(1 << 20) // math.isqrt(grade ** slope) + 1 for grade in range(1, count + 1)]
    largest = reach if full else min(reach, max(-(-total // count), total * weights[0] // sum(weights)))
    least = 1 if total - largest >= count - 1 else 0
    given, surplus = [largest] + [least] * (count - 1), total - largest - least * (count - 1)
    while surplus > 0:
        movable = [i for i in range(1, count) if given[i] < largest] or [i for i in range(1, count) if given[i] < reach]
        pool, left = sum([weights[i] for i in movable]), surplus
        for i in movable:
            extra = min(reach - given[i], max(1, left * weights[i] // pool), surplus)
            given[i] = given[i] + extra
            surplus = surplus - extra
    return np.array(given)


def bell_draw(stream_key, dims, scale, limit, cuts=(), kind=jnp.bfloat16):
    array = jax.random.normal(stream_key, dims, jnp.float32) * scale
    if len(cuts) > 0:
        array = block_scale(stream_key, dims, cuts, -0.22, 0.18) * array
    return jnp.clip(array, min=-limit, max=limit).astype(kind)


def noise_with(own_key, dims, deviation, bound, cuts, heavy, dtype=jnp.bfloat16):
    array = deviation * jax.random.normal(own_key, dims, jnp.float32)
    if cuts:
        array = array * block_scale(own_key, dims, cuts, -0.22, 0.18)
    return jnp.clip(raised(array, jax.random.fold_in(own_key, 3), *heavy), -bound, bound).astype(dtype)


def setup_inputs(seed: int = 0, part: int = 0) -> dict:
    key_list = jax.random.split(jax.random.key(seed), 22)
    part_keys = jax.random.split(jax.random.fold_in(key_list[21], part), 22)
    tokens = bell_draw(part_keys[0], (TOKENS, D), 1.0, 6.0, ((0, 4),))
    conv_state = bell_draw(part_keys[1], (TOKENS, CONV_W - 1, LRU), 1.0, 6.0, ((0, 4), (2, 4)))
    state_h = bell_draw(part_keys[2], (TOKENS, LRU), 1.0, 6.0, ((0, 4), (1, 4)), jnp.float32)
    mixer_gain = jnp.clip(1.0 + 0.18 * jax.random.normal(key_list[3], (D,), jnp.float32), 0.099609375, 1.8984375).astype(jnp.bfloat16)
    expert_gain = jnp.clip(1.0 + 0.18 * jax.random.normal(key_list[4], (D,), jnp.float32), 0.099609375, 1.8984375).astype(jnp.bfloat16)
    input_proj = bell_draw(key_list[5], (D, LRU), D ** -0.5, 0.125, ((0, 4), (1, 4)))
    branch_proj = bell_draw(key_list[6], (D, LRU), D ** -0.5, 0.125, ((0, 4), (1, 4)))
    conv_taps = bell_draw(key_list[7], (CONV_W, LRU), CONV_W ** -0.5, 3.0, ((1, 4),))
    write_map = bell_draw(key_list[8], (LRU_HEADS, HEAD_W, HEAD_W), HEAD_W ** -0.5, 0.5, ((0, 4),))
    decay_map = bell_draw(key_list[9], (LRU_HEADS, HEAD_W, HEAD_W), HEAD_W ** -0.5, 0.5, ((0, 4),))
    decay_rate = jnp.clip(jnp.exp(math.log(0.4) - 3.6888795 * jax.random.uniform(key_list[10], (LRU,), jnp.float32) ** block_scale(key_list[10], (LRU,), ((0, 4),), -0.2, 0.2)), 0.01, 0.4)
    output_proj = bell_draw(key_list[11], (LRU, D), LRU ** -0.5, 0.1875, ((0, 4),))
    route_ids_keys = jax.random.split(jax.random.fold_in(part_keys[12], 1), TOKENS // TOKENS)
    route_ids_turns = jax.random.permutation(jax.random.fold_in(part_keys[12], 3), TOKENS // TOKENS)
    route_ids = jax.vmap(lambda own, number: routed_block(jax.random.fold_in(part_keys[12], 2), own, number, TOKENS, EXPERTS, TOPK, CAP, 2))(route_ids_keys, route_ids_turns).reshape((TOKENS, TOPK))
    route_scores = jnp.clip(jnp.exp(jax.random.uniform(part_keys[13], (TOKENS, TOPK), jnp.float32, math.log(0.5), math.log(4.0))), 0.5, 4.0)
    expert_gate = bell_draw(key_list[14], (EXPERTS, D, EXP_FF), D ** -0.5, 0.125, ((0, 4), (2, 4)))
    expert_up = bell_draw(key_list[15], (EXPERTS, D, EXP_FF), D ** -0.5, 0.125, ((0, 4), (2, 4)))
    expert_down = bell_draw(key_list[16], (EXPERTS, EXP_FF, D), EXP_FF ** -0.5, 0.1875, ((0, 4), (1, 4)))
    branch_gate = bell_draw(key_list[17], (D,), D ** -0.5, 0.125)
    shared_gate = bell_draw(key_list[18], (D, DENSE_FF), D ** -0.5, 0.125, ((1, 16),))
    shared_up = bell_draw(key_list[19], (D, DENSE_FF), D ** -0.5, 0.125, ((1, 16),))
    shared_down = noise_with(key_list[20], (DENSE_FF, D), DENSE_FF ** -0.5, 0.0625, ((0, 16),), (0, 1, 16, 2.0))
    return {"tokens": tokens, "conv_state": conv_state, "state_h": state_h, "mixer_gain": mixer_gain, "expert_gain": expert_gain, "input_proj": input_proj, "branch_proj": branch_proj, "conv_taps": conv_taps, "write_map": write_map, "decay_map": decay_map, "decay_rate": decay_rate, "output_proj": output_proj, "route_ids": route_ids, "route_scores": route_scores, "expert_gate": expert_gate, "expert_up": expert_up, "expert_down": expert_down, "branch_gate": branch_gate, "shared_gate": shared_gate, "shared_up": shared_up, "shared_down": shared_down}


def rms_norm(array_in, gain_vec):
    values = array_in.astype(jnp.float32)
    scaled = values * lax.rsqrt(lax.optimization_barrier(jnp.mean(values * values, axis=-1, keepdims=True)) + 1e-06)
    return (scaled * gain_vec.astype(jnp.float32)).astype(jnp.bfloat16)

def reference(tokens, conv_state, state_h, mixer_gain, expert_gain, input_proj, branch_proj, conv_taps, write_map, decay_map, decay_rate, output_proj, route_ids, route_scores, expert_gate, expert_up, expert_down, branch_gate, shared_gate, shared_up, shared_down):
    normed = rms_norm(tokens, mixer_gain)
    inner_x = jnp.dot(normed, input_proj, preferred_element_type=jnp.float32).astype(jnp.bfloat16)
    branch_x = jnp.dot(normed, branch_proj, preferred_element_type=jnp.float32).astype(jnp.bfloat16)
    window_rows = jnp.concatenate([conv_state, inner_x[:, None, :]], axis=1)
    convolved = lax.optimization_barrier(jnp.sum(window_rows.astype(jnp.float32) * conv_taps.astype(jnp.float32)[None], axis=1))
    conv_round = convolved.astype(jnp.bfloat16).astype(jnp.float32).reshape(TOKENS, LRU_HEADS, HEAD_W)
    write_gate = jax.nn.sigmoid(jnp.einsum('thi,hij->thj', conv_round, write_map.astype(jnp.float32)).reshape(TOKENS, LRU))
    decay_gate = jax.nn.sigmoid(jnp.einsum('thi,hij->thj', conv_round, decay_map.astype(jnp.float32)).reshape(TOKENS, LRU))
    log_keep = -8.0 * decay_gate * decay_rate
    state_next = jnp.exp(log_keep) * state_h + jnp.sqrt(-jnp.expm1(2.0 * log_keep)) * write_gate * convolved
    mixed = (state_next * jax.nn.gelu(branch_x.astype(jnp.float32))).astype(jnp.bfloat16)
    mixed_out = jnp.dot(mixed, output_proj, preferred_element_type=jnp.float32)
    resid = (tokens.astype(jnp.float32) + mixed_out).astype(jnp.bfloat16)
    normed2 = rms_norm(resid, expert_gain)
    route_weight = route_scores / lax.optimization_barrier(jnp.sum(route_scores, axis=1, keepdims=True))

    def add_expert(expert_idx, running):
        gate_pre = jnp.dot(normed2, expert_gate[expert_idx], preferred_element_type=jnp.float32)
        up_pre = jnp.dot(normed2, expert_up[expert_idx], preferred_element_type=jnp.float32)
        hidden = (jax.nn.silu(gate_pre) * up_pre).astype(jnp.bfloat16)
        expert_out = jnp.dot(hidden, expert_down[expert_idx], preferred_element_type=jnp.float32)
        chosen = lax.optimization_barrier(jnp.sum(jnp.where(route_ids == expert_idx, route_weight, jnp.zeros_like(route_weight)), axis=1))
        return running + chosen[:, None] * expert_out
    expert_sum = lax.fori_loop(0, EXPERTS, add_expert, jnp.zeros((TOKENS, D), jnp.float32))
    dense_hidden = (jax.nn.silu(jnp.dot(normed2, shared_gate, preferred_element_type=jnp.float32)) * jnp.dot(normed2, shared_up, preferred_element_type=jnp.float32)).astype(jnp.bfloat16)
    branch_mix = jax.nn.sigmoid(jnp.dot(normed2, branch_gate, preferred_element_type=jnp.float32))
    dense_out = jnp.dot(dense_hidden, shared_down, preferred_element_type=jnp.float32)
    result = (resid.astype(jnp.float32) + expert_sum + branch_mix[:, None] * dense_out).astype(jnp.bfloat16)
    conv_next = window_rows[:, 1:]
    return (result, state_next, conv_next)
```

```python
import functools

import jax
import jax.numpy as jnp
from jax import lax
from jax.experimental import pallas as pl
from jax.experimental.pallas import tpu as pltpu
from jax.sharding import PartitionSpec as P

MESH = pl.DeviceIdType.MESH
F32 = jnp.float32
BF16 = jnp.bfloat16


def each(count, step):
    if count <= 16:
        for number in range(count):
            step(number)
    else:

        def body(number, carry):
            step(number)
            return carry

        lax.fori_loop(0, count, body, 0)


def mm(left, right):
    return jnp.dot(left, right, preferred_element_type=F32)


def silu(value):
    return value * jax.nn.sigmoid(value)


def layer_kernel(
    ep,
    tp,
    tokens,
    conv_state,
    state_h,
    mixer_gain,
    expert_gain,
    input_proj,
    branch_proj,
    conv_taps,
    write_map,
    decay_map,
    decay_rate,
    output_proj,
    route_ids,
    route_scores,
    expert_gate,
    expert_up,
    expert_down,
    branch_gate,
    shared_gate,
    shared_up,
    shared_down,
    result_out,
    state_out,
    conv_out,
    tok_all,
    conv_all,
    state_all,
    mgain,
    egain,
    iproj,
    bproj,
    taps,
    wmap,
    dmap,
    rate,
    oproj,
    ids,
    scores,
    eg_w,
    eu_w,
    ed_w,
    bgate,
    sg_w,
    su_w,
    sd_w,
    norm_s,
    part_in,
    part_out,
    part_send,
    part_recv,
    resid_s,
    next_s,
    inner_s,
    local_sem,
    tok_ss,
    tok_rs,
    conv_ss,
    conv_rs,
    state_ss,
    state_rs,
    in_ss,
    in_rs,
    out_ss,
    out_rs,
    last_ss,
    last_rs,
):
    me_e = lax.axis_index("ep")
    me_t = lax.axis_index("tp")
    rows = ep
    width = tok_all.shape[-1]
    channels = iproj.shape[1]
    depth = iproj.shape[0]
    col_width = part_send.shape[-1]
    me_flat = me_e * tp + me_t

    small = [
        (tokens, tok_all.at[me_e]),
        (conv_state.at[0], conv_all.at[me_e]),
        (state_h, state_all.at[me_e]),
        (mixer_gain, mgain),
        (input_proj, iproj),
        (branch_proj, bproj),
        (conv_taps, taps),
        (write_map, wmap),
        (decay_map, dmap),
        (decay_rate, rate),
        (output_proj, oproj),
        (expert_gain, egain),
        (route_ids, ids),
        (route_scores, scores),
        (branch_gate, bgate),
    ]
    large = [
        (shared_gate, sg_w),
        (shared_up, su_w),
        (expert_gate.at[0], eg_w),
        (expert_up.at[0], eu_w),
        (expert_down.at[0], ed_w),
        (shared_down, sd_w),
    ]
    local = [
        pltpu.make_async_copy(src, dst, local_sem.at[number])
        for number, (src, dst) in enumerate(small + large)
    ]
    (
        c_tok,
        c_conv,
        c_state,
        c_mgain,
        c_iproj,
        c_bproj,
        c_taps,
        c_wmap,
        c_dmap,
        c_rate,
        c_oproj,
        c_egain,
        c_ids,
        c_scores,
        c_bgate,
        c_sg,
        c_su,
        c_eg,
        c_eu,
        c_ed,
        c_sd,
    ) = local
    for copy in local[: len(small)]:
        copy.start()

    barrier = pltpu.get_barrier_semaphore()

    def greet(number):
        flat = lax.rem(me_flat + 1 + number, ep * tp)
        pl.semaphore_signal(
            barrier,
            inc=1,
            device_id={"ep": flat // tp, "tp": lax.rem(flat, tp)},
            device_id_type=MESH,
        )

    each(ep * tp - 1, greet)
    pl.semaphore_wait(barrier, ep * tp - 1)

    def over_ep(buf, ssem, rsem, slot, peer):
        return pltpu.make_async_remote_copy(
            src_ref=buf.at[slot],
            dst_ref=buf.at[slot],
            send_sem=ssem.at[peer],
            recv_sem=rsem.at[slot],
            device_id={"ep": peer},
            device_id_type=MESH,
        )

    def over_tp(buf, ssem, rsem, slot, peer):
        return pltpu.make_async_remote_copy(
            src_ref=buf.at[slot],
            dst_ref=buf.at[slot],
            send_sem=ssem.at[peer],
            recv_sem=rsem.at[slot],
            device_id={"tp": peer},
            device_id_type=MESH,
        )

    def ep_peer(number):
        return lax.rem(me_e + 1 + number, ep)

    def tp_peer(number):
        return lax.rem(me_t + 1 + number, tp)

    def send_ep(buf, ssem, rsem):
        each(ep - 1, lambda n: over_ep(buf, ssem, rsem, me_e, ep_peer(n)).start())

    def recv_ep(buf, ssem, rsem):
        each(ep - 1, lambda n: over_ep(buf, ssem, rsem, ep_peer(n), ep_peer(n)).wait_recv())

    def sent_ep(buf, ssem, rsem):
        each(ep - 1, lambda n: over_ep(buf, ssem, rsem, me_e, ep_peer(n)).wait_send())

    c_tok.wait()
    send_ep(tok_all, tok_ss, tok_rs)
    c_conv.wait()
    send_ep(conv_all, conv_ss, conv_rs)
    c_state.wait()
    send_ep(state_all, state_ss, state_rs)
    for copy in local[len(small) :]:
        copy.start()

    c_mgain.wait()
    c_iproj.wait()
    c_bproj.wait()
    recv_ep(tok_all, tok_ss, tok_rs)
    tok = jnp.concatenate([tok_all[row].astype(F32) for row in range(rows)], axis=0)
    scale = lax.rsqrt(jnp.mean(tok * tok, axis=-1, keepdims=True) + 1e-06)
    normed = tok * scale * mgain[...].astype(F32).reshape(1, width)
    if depth % 128 == 0:
        norm_s[...] = normed
        mine = norm_s[:, pl.ds(pl.multiple_of(me_e * depth, depth), depth)]
    else:
        mine = pltpu.roll(normed, lax.rem(width - me_e * depth, width), 1)[:, :depth]
    mine = mine.astype(BF16)
    part_in[me_e] = jnp.concatenate([mm(mine, iproj[...]), mm(mine, bproj[...])], axis=1).astype(
        BF16
    )
    send_ep(part_in, in_ss, in_rs)

    c_taps.wait()
    c_wmap.wait()
    c_dmap.wait()
    c_rate.wait()
    c_oproj.wait()
    recv_ep(conv_all, conv_ss, conv_rs)
    recv_ep(state_all, state_ss, state_rs)
    tap = taps[...].astype(F32)
    past = tap.shape[0] - 1
    history = jnp.concatenate(
        [
            jnp.sum(conv_all[row].astype(F32) * tap[:past], axis=0, keepdims=True)
            for row in range(rows)
        ],
        axis=0,
    )
    state = jnp.concatenate([state_all[row] for row in range(rows)], axis=0)
    rates = rate[...].reshape(1, channels)

    recv_ep(part_in, in_ss, in_rs)
    projected = jnp.sum(part_in[...].astype(F32), axis=0)
    inner_x = projected[:, :channels].astype(BF16).astype(F32)
    branch_x = projected[:, channels:].astype(BF16).astype(F32)
    convolved = history + tap[past:] * inner_x
    conv_round = convolved.astype(BF16)
    heads, head_width = wmap.shape[0], wmap.shape[1]

    def by_head(maps):
        return jnp.concatenate(
            [
                mm(conv_round[:, h * head_width : (h + 1) * head_width], maps[h])
                for h in range(heads)
            ],
            axis=1,
        )

    write_gate = jax.nn.sigmoid(by_head(wmap))
    decay_gate = jax.nn.sigmoid(by_head(dmap))
    forget = 8.0 * decay_gate * rates
    bent = jnp.tanh(forget)
    state_next = (
        jnp.exp(-forget) * state
        + jnp.sqrt(2.0 * bent / (1.0 + bent)) * write_gate * convolved
    )
    mixed = (state_next * jax.nn.gelu(branch_x)).astype(BF16)
    part_out[me_t] = mm(mixed, oproj[...]).astype(BF16)
    each(tp - 1, lambda n: over_tp(part_out, out_ss, out_rs, me_t, tp_peer(n)).start())

    for row in range(rows):
        next_s[row] = state_next[row : row + 1]
        inner_s[row] = inner_x[row : row + 1]
    state_out[...] = next_s[me_e]
    conv_out[0] = jnp.concatenate([conv_all[me_e].astype(F32)[1:], inner_s[me_e]], axis=0).astype(
        BF16
    )
    c_egain.wait()
    c_ids.wait()
    c_scores.wait()
    c_bgate.wait()
    score = scores[...]
    share = score / jnp.sum(score, axis=1, keepdims=True)
    chosen = jnp.sum(jnp.where(ids[...] == me_e, share, 0.0), axis=1, keepdims=True)
    gain2 = egain[...].astype(F32).reshape(1, width)
    mixer = bgate[...].astype(F32).reshape(1, width)
    for copy in local[len(small) :]:
        copy.wait()

    each(tp - 1, lambda n: over_tp(part_out, out_ss, out_rs, tp_peer(n), tp_peer(n)).wait_recv())
    resid = (tok + jnp.sum(part_out[...].astype(F32), axis=0)).astype(BF16).astype(F32)
    scale2 = lax.rsqrt(jnp.mean(resid * resid, axis=-1, keepdims=True) + 1e-06)
    normed2 = (resid * scale2 * gain2).astype(BF16)
    dense = (silu(mm(normed2, sg_w[...])) * mm(normed2, su_w[...])).astype(BF16)
    hidden = (silu(mm(normed2, eg_w[...])) * mm(normed2, eu_w[...])).astype(BF16)
    blend = jax.nn.sigmoid(jnp.sum(normed2.astype(F32) * mixer, axis=-1, keepdims=True))

    def last(col, row, slot):
        return pltpu.make_async_remote_copy(
            src_ref=part_send.at[col, row],
            dst_ref=part_recv.at[slot],
            send_sem=last_ss.at[row * tp + col],
            recv_sem=last_rs.at[slot],
            device_id={"ep": row, "tp": col},
            device_id_type=MESH,
        )

    for step in range(tp):
        col = lax.rem(me_t + 1 + step, tp)
        at = pl.ds(pl.multiple_of(col * col_width, col_width), col_width)
        sums = (chosen * mm(hidden, ed_w[:, at]) + blend * mm(dense, sd_w[:, at])).astype(BF16)
        for row in range(rows):
            part_send[col, row] = sums[row : row + 1]
        count = ep - 1 if step == tp - 1 else ep
        each(count, lambda n: last(col, ep_peer(n), me_flat).start())
    part_recv[me_flat] = part_send[me_t, me_e]
    for row in range(rows):
        resid_s[row] = resid[row : row + 1]
    own = resid_s[me_e, :, pl.ds(pl.multiple_of(me_t * col_width, col_width), col_width)]

    def other(number):
        flat = lax.rem(me_flat + 1 + number, ep * tp)
        return flat // tp, lax.rem(flat, tp), flat

    def recv_last(number):
        row, col, flat = other(number)
        last(col, row, flat).wait_recv()

    def sent_last(number):
        row, col, flat = other(number)
        last(col, row, flat).wait_send()

    each(ep * tp - 1, recv_last)
    total = own + jnp.sum(part_recv[...].astype(F32), axis=0)
    result_out[...] = total.astype(BF16)

    sent_ep(tok_all, tok_ss, tok_rs)
    sent_ep(conv_all, conv_ss, conv_rs)
    sent_ep(state_all, state_ss, state_rs)
    sent_ep(part_in, in_ss, in_rs)
    each(tp - 1, lambda n: over_tp(part_out, out_ss, out_rs, me_t, tp_peer(n)).wait_send())
    each(ep * tp - 1, sent_last)


def on_device(ep, tp, *args):
    (
        tokens,
        conv_state,
        state_h,
        mixer_gain,
        expert_gain,
        input_proj,
        branch_proj,
        conv_taps,
        write_map,
        decay_map,
        decay_rate,
        output_proj,
        route_ids,
        route_scores,
        expert_gate,
        expert_up,
        expert_down,
        branch_gate,
        shared_gate,
        shared_up,
        shared_down,
    ) = args
    assert tokens.shape[0] == 1
    rows = ep
    width = tokens.shape[1]
    channels = state_h.shape[1]
    col_width = width // tp
    past = conv_state.shape[1]

    def like(array):
        return pltpu.VMEM(array.shape, array.dtype)

    def inner(array):
        return pltpu.VMEM(array.shape[1:], array.dtype)

    dma = pltpu.SemaphoreType.DMA
    scratch = [
        pltpu.VMEM((rows, 1, width), BF16),
        pltpu.VMEM((rows, past, channels), BF16),
        pltpu.VMEM((rows, 1, channels), F32),
        like(mixer_gain),
        like(expert_gain),
        like(input_proj),
        like(branch_proj),
        like(conv_taps),
        like(write_map),
        like(decay_map),
        like(decay_rate),
        like(output_proj),
        like(route_ids),
        like(route_scores),
        inner(expert_gate),
        inner(expert_up),
        inner(expert_down),
        like(branch_gate),
        like(shared_gate),
        like(shared_up),
        like(shared_down),
        pltpu.VMEM((rows, width), F32),
        pltpu.VMEM((ep, rows, 2 * channels), BF16),
        pltpu.VMEM((tp, rows, width), BF16),
        pltpu.VMEM((tp, rows, 1, col_width), BF16),
        pltpu.VMEM((ep * tp, 1, col_width), BF16),
        pltpu.VMEM((rows, 1, width), F32),
        pltpu.VMEM((rows, 1, channels), F32),
        pltpu.VMEM((rows, 1, channels), F32),
        dma((len(args),)),
    ]
    scratch += [dma((ep,))] * 8 + [dma((tp,))] * 2 + [dma((ep * tp,))] * 2
    return pl.pallas_call(
        functools.partial(layer_kernel, ep, tp),
        out_shape=(
            jax.ShapeDtypeStruct((1, col_width), BF16),
            jax.ShapeDtypeStruct((1, channels), F32),
            jax.ShapeDtypeStruct((1, past, channels), BF16),
        ),
        in_specs=[pl.BlockSpec(memory_space=pl.ANY)] * len(args),
        out_specs=[pl.BlockSpec(memory_space=pltpu.VMEM)] * 3,
        scratch_shapes=scratch,
        compiler_params=pltpu.CompilerParams(
            collective_id=0, has_side_effects=True, vmem_limit_bytes=60 * 1024 * 1024
        ),
    )(*args)


def solution(mesh):
    placed = (
        P(("grp", "ep"), None),
        P(("grp", "ep"), None, "tp"),
        P(("grp", "ep"), "tp"),
        P(),
        P(),
        P("ep", "tp"),
        P("ep", "tp"),
        P(None, "tp"),
        P("tp", None, None),
        P("tp", None, None),
        P("tp"),
        P("tp", None),
        P("grp", None),
        P("grp", None),
        P("ep", None, "tp"),
        P("ep", None, "tp"),
        P("ep", "tp", None),
        P(),
        P(None, ("ep", "tp")),
        P(None, ("ep", "tp")),
        P(("ep", "tp"), None),
    )
    return jax.shard_map(
        functools.partial(on_device, mesh.shape["ep"], mesh.shape["tp"]),
        mesh=mesh,
        in_specs=placed,
        out_specs=(P(("grp", "ep"), "tp"), P(("grp", "ep"), "tp"), P(("grp", "ep"), None, "tp")),
        check_vma=False,
    )
```

```python
import functools

import jax
import jax.numpy as jnp
from jax import lax
from jax.experimental import pallas as pl
from jax.experimental.pallas import tpu as pltpu
from jax.sharding import PartitionSpec as P

MESH = pl.DeviceIdType.MESH
F32 = jnp.float32
BF16 = jnp.bfloat16


def each(count, step):
    if count <= 16:
        for number in range(count):
            step(number)
    else:

        def body(number, carry):
            step(number)
            return carry

        lax.fori_loop(0, count, body, 0)


def mm(left, right):
    return jnp.dot(left, right, preferred_element_type=F32)


def silu(value):
    return value * jax.nn.sigmoid(value)


def layer_kernel(
    ep,
    tp,
    tokens,
    conv_state,
    state_h,
    mixer_gain,
    expert_gain,
    input_proj,
    branch_proj,
    conv_taps,
    write_map,
    decay_map,
    decay_rate,
    output_proj,
    route_ids,
    route_scores,
    expert_gate,
    expert_up,
    expert_down,
    branch_gate,
    shared_gate,
    shared_up,
    shared_down,
    result_out,
    state_out,
    conv_out,
    tok_all,
    conv_all,
    state_all,
    mgain,
    egain,
    iproj,
    bproj,
    taps,
    wmap,
    dmap,
    rate,
    oproj,
    ids,
    scores,
    eg_w,
    eu_w,
    ed_w,
    bgate,
    sg_w,
    su_w,
    sd_w,
    norm_s,
    part_in,
    part_out,
    part_send,
    part_recv,
    resid_s,
    next_s,
    inner_s,
    local_sem,
    tok_ss,
    tok_rs,
    conv_ss,
    conv_rs,
    state_ss,
    state_rs,
    in_ss,
    in_rs,
    out_ss,
    out_rs,
    last_ss,
    last_rs,
):
    me_e = lax.axis_index("ep")
    me_t = lax.axis_index("tp")
    rows = ep
    width = tok_all.shape[-1]
    channels = iproj.shape[1]
    depth = iproj.shape[0]
    col_width = part_send.shape[-1]
    me_flat = me_e * tp + me_t

    small = [
        (tokens, tok_all.at[me_e]),
        (conv_state.at[0], conv_all.at[me_e]),
        (state_h, state_all.at[me_e]),
        (mixer_gain, mgain),
        (input_proj, iproj),
        (branch_proj, bproj),
        (conv_taps, taps),
        (write_map, wmap),
        (decay_map, dmap),
        (decay_rate, rate),
        (output_proj, oproj),
        (expert_gain, egain),
        (route_ids, ids),
        (route_scores, scores),
        (branch_gate, bgate),
    ]
    large = [
        (shared_gate, sg_w),
        (shared_up, su_w),
        (expert_gate.at[0], eg_w),
        (expert_up.at[0], eu_w),
        (expert_down.at[0], ed_w),
        (shared_down, sd_w),
    ]
    local = [
        pltpu.make_async_copy(src, dst, local_sem.at[number])
        for number, (src, dst) in enumerate(small + large)
    ]
    (
        c_tok,
        c_conv,
        c_state,
        c_mgain,
        c_iproj,
        c_bproj,
        c_taps,
        c_wmap,
        c_dmap,
        c_rate,
        c_oproj,
        c_egain,
        c_ids,
        c_scores,
        c_bgate,
        c_sg,
        c_su,
        c_eg,
        c_eu,
        c_ed,
        c_sd,
    ) = local
    for copy in local[: len(small)]:
        copy.start()

    barrier = pltpu.get_barrier_semaphore()

    def greet(number):
        flat = lax.rem(me_flat + 1 + number, ep * tp)
        pl.semaphore_signal(
            barrier,
            inc=1,
            device_id={"ep": flat // tp, "tp": lax.rem(flat, tp)},
            device_id_type=MESH,
        )

    each(ep * tp - 1, greet)
    pl.semaphore_wait(barrier, ep * tp - 1)

    def over_ep(buf, ssem, rsem, slot, peer):
        return pltpu.make_async_remote_copy(
            src_ref=buf.at[slot],
            dst_ref=buf.at[slot],
            send_sem=ssem.at[peer],
            recv_sem=rsem.at[slot],
            device_id={"ep": peer},
            device_id_type=MESH,
        )

    def over_tp(buf, ssem, rsem, slot, peer):
        return pltpu.make_async_remote_copy(
            src_ref=buf.at[slot],
            dst_ref=buf.at[slot],
            send_sem=ssem.at[peer],
            recv_sem=rsem.at[slot],
            device_id={"tp": peer},
            device_id_type=MESH,
        )

    def ep_peer(number):
        return lax.rem(me_e + 1 + number, ep)

    def tp_peer(number):
        return lax.rem(me_t + 1 + number, tp)

    def send_ep(buf, ssem, rsem):
        each(ep - 1, lambda n: over_ep(buf, ssem, rsem, me_e, ep_peer(n)).start())

    def recv_ep(buf, ssem, rsem):
        each(ep - 1, lambda n: over_ep(buf, ssem, rsem, ep_peer(n), ep_peer(n)).wait_recv())

    def sent_ep(buf, ssem, rsem):
        each(ep - 1, lambda n: over_ep(buf, ssem, rsem, me_e, ep_peer(n)).wait_send())

    c_tok.wait()
    send_ep(tok_all, tok_ss, tok_rs)
    c_conv.wait()
    send_ep(conv_all, conv_ss, conv_rs)
    c_state.wait()
    send_ep(state_all, state_ss, state_rs)
    for copy in local[len(small) :]:
        copy.start()

    c_mgain.wait()
    c_iproj.wait()
    c_bproj.wait()
    recv_ep(tok_all, tok_ss, tok_rs)
    tok = jnp.concatenate([tok_all[row].astype(F32) for row in range(rows)], axis=0)
    scale = lax.rsqrt(jnp.mean(tok * tok, axis=-1, keepdims=True) + 1e-06)
    normed = tok * scale * mgain[...].astype(F32).reshape(1, width)
    if depth % 128 == 0:
        norm_s[...] = normed
        mine = norm_s[:, pl.ds(pl.multiple_of(me_e * depth, depth), depth)]
    else:
        mine = pltpu.roll(normed, lax.rem(width - me_e * depth, width), 1)[:, :depth]
    mine = mine.astype(BF16)
    part_in[me_e] = jnp.concatenate([mm(mine, iproj[...]), mm(mine, bproj[...])], axis=1).astype(
        BF16
    )
    send_ep(part_in, in_ss, in_rs)

    c_taps.wait()
    c_wmap.wait()
    c_dmap.wait()
    c_rate.wait()
    c_oproj.wait()
    recv_ep(conv_all, conv_ss, conv_rs)
    recv_ep(state_all, state_ss, state_rs)
    tap = taps[...].astype(F32)
    past = tap.shape[0] - 1
    history = jnp.concatenate(
        [
            jnp.sum(conv_all[row].astype(F32) * tap[:past], axis=0, keepdims=True)
            for row in range(rows)
        ],
        axis=0,
    )
    state = jnp.concatenate([state_all[row] for row in range(rows)], axis=0)
    rates = rate[...].reshape(1, channels)

    recv_ep(part_in, in_ss, in_rs)
    projected = jnp.sum(part_in[...].astype(F32), axis=0)
    inner_x = projected[:, :channels].astype(BF16).astype(F32)
    branch_x = projected[:, channels:].astype(BF16).astype(F32)
    convolved = history + tap[past:] * inner_x
    conv_round = convolved.astype(BF16)
    heads, head_width = wmap.shape[0], wmap.shape[1]

    def by_head(maps):
        return jnp.concatenate(
            [
                mm(conv_round[:, h * head_width : (h + 1) * head_width], maps[h])
                for h in range(heads)
            ],
            axis=1,
        )

    write_gate = jax.nn.sigmoid(by_head(wmap))
    decay_gate = jax.nn.sigmoid(by_head(dmap))
    forget = 8.0 * decay_gate * rates
    bent = jnp.tanh(forget)
    state_next = (
        jnp.exp(-forget) * state
        + jnp.sqrt(2.0 * bent / (1.0 + bent)) * write_gate * convolved
    )
    mixed = (state_next * jax.nn.gelu(branch_x)).astype(BF16)
    part_out[me_t] = mm(mixed, oproj[...]).astype(BF16)
    each(tp - 1, lambda n: over_tp(part_out, out_ss, out_rs, me_t, tp_peer(n)).start())

    for row in range(rows):
        next_s[row] = state_next[row : row + 1]
        inner_s[row] = inner_x[row : row + 1]
    state_out[...] = next_s[me_e]
    conv_out[0] = jnp.concatenate([conv_all[me_e].astype(F32)[1:], inner_s[me_e]], axis=0).astype(
        BF16
    )
    c_egain.wait()
    c_ids.wait()
    c_scores.wait()
    c_bgate.wait()
    score = scores[...]
    share = score / jnp.sum(score, axis=0, keepdims=True)
    chosen = jnp.sum(jnp.where(ids[...] == me_e, share, 0.0), axis=0, keepdims=True)
    square = (rows, rows)
    diagonal = lax.broadcasted_iota(jnp.int32, square, 0) == lax.broadcasted_iota(
        jnp.int32, square, 1
    )
    chosen = jnp.sum(jnp.where(diagonal, chosen, 0.0), axis=1, keepdims=True)
    gain2 = egain[...].astype(F32).reshape(1, width)
    mixer = bgate[...].astype(F32).reshape(1, width)
    for copy in local[len(small) :]:
        copy.wait()

    each(tp - 1, lambda n: over_tp(part_out, out_ss, out_rs, tp_peer(n), tp_peer(n)).wait_recv())
    resid = (tok + jnp.sum(part_out[...].astype(F32), axis=0)).astype(BF16).astype(F32)
    scale2 = lax.rsqrt(jnp.mean(resid * resid, axis=-1, keepdims=True) + 1e-06)
    normed2 = (resid * scale2 * gain2).astype(BF16)
    dense = (silu(mm(normed2, sg_w[...])) * mm(normed2, su_w[...])).astype(BF16)
    hidden = (silu(mm(normed2, eg_w[...])) * mm(normed2, eu_w[...])).astype(BF16)
    blend = jax.nn.sigmoid(jnp.sum(normed2.astype(F32) * mixer, axis=-1, keepdims=True))

    def last(col, row, slot):
        return pltpu.make_async_remote_copy(
            src_ref=part_send.at[col, row],
            dst_ref=part_recv.at[slot],
            send_sem=last_ss.at[row * tp + col],
            recv_sem=last_rs.at[slot],
            device_id={"ep": row, "tp": col},
            device_id_type=MESH,
        )

    for step in range(tp):
        col = lax.rem(me_t + 1 + step, tp)
        at = pl.ds(pl.multiple_of(col * col_width, col_width), col_width)
        sums = (chosen * mm(hidden, ed_w[:, at]) + blend * mm(dense, sd_w[:, at])).astype(BF16)
        for row in range(rows):
            part_send[col, row] = sums[row : row + 1]
        count = ep - 1 if step == tp - 1 else ep
        each(count, lambda n: last(col, ep_peer(n), me_flat).start())
    part_recv[me_flat] = part_send[me_t, me_e]
    for row in range(rows):
        resid_s[row] = resid[row : row + 1]
    own = resid_s[me_e, :, pl.ds(pl.multiple_of(me_t * col_width, col_width), col_width)]

    def other(number):
        flat = lax.rem(me_flat + 1 + number, ep * tp)
        return flat // tp, lax.rem(flat, tp), flat

    def recv_last(number):
        row, col, flat = other(number)
        last(col, row, flat).wait_recv()

    def sent_last(number):
        row, col, flat = other(number)
        last(col, row, flat).wait_send()

    each(ep * tp - 1, recv_last)
    total = own + jnp.sum(part_recv[...].astype(F32), axis=0)
    result_out[...] = total.astype(BF16)

    sent_ep(tok_all, tok_ss, tok_rs)
    sent_ep(conv_all, conv_ss, conv_rs)
    sent_ep(state_all, state_ss, state_rs)
    sent_ep(part_in, in_ss, in_rs)
    each(tp - 1, lambda n: over_tp(part_out, out_ss, out_rs, me_t, tp_peer(n)).wait_send())
    each(ep * tp - 1, sent_last)


def hand_over(result, state, conv, result_out, state_out, conv_out):
    result_out[...] = result[...]
    state_out[...] = state[...]
    conv_out[...] = conv[...]


def on_device(ep, tp, *args):
    (
        tokens,
        conv_state,
        state_h,
        mixer_gain,
        expert_gain,
        input_proj,
        branch_proj,
        conv_taps,
        write_map,
        decay_map,
        decay_rate,
        output_proj,
        route_ids,
        route_scores,
        expert_gate,
        expert_up,
        expert_down,
        branch_gate,
        shared_gate,
        shared_up,
        shared_down,
    ) = args
    assert tokens.shape[0] == 1
    route_ids, route_scores = route_ids.T, route_scores.T
    args = args[:12] + (route_ids, route_scores) + args[14:]
    rows = ep
    width = tokens.shape[1]
    channels = state_h.shape[1]
    col_width = width // tp
    past = conv_state.shape[1]

    def like(array):
        return pltpu.VMEM(array.shape, array.dtype)

    def inner(array):
        return pltpu.VMEM(array.shape[1:], array.dtype)

    dma = pltpu.SemaphoreType.DMA
    scratch = [
        pltpu.VMEM((rows, 1, width), BF16),
        pltpu.VMEM((rows, past, channels), BF16),
        pltpu.VMEM((rows, 1, channels), F32),
        like(mixer_gain),
        like(expert_gain),
        like(input_proj),
        like(branch_proj),
        like(conv_taps),
        like(write_map),
        like(decay_map),
        like(decay_rate),
        like(output_proj),
        like(route_ids),
        like(route_scores),
        inner(expert_gate),
        inner(expert_up),
        inner(expert_down),
        like(branch_gate),
        like(shared_gate),
        like(shared_up),
        like(shared_down),
        pltpu.VMEM((rows, width), F32),
        pltpu.VMEM((ep, rows, 2 * channels), BF16),
        pltpu.VMEM((tp, rows, width), BF16),
        pltpu.VMEM((tp, rows, 1, col_width), BF16),
        pltpu.VMEM((ep * tp, 1, col_width), BF16),
        pltpu.VMEM((rows, 1, width), F32),
        pltpu.VMEM((rows, 1, channels), F32),
        pltpu.VMEM((rows, 1, channels), F32),
        dma((len(args),)),
    ]
    scratch += [dma((ep,))] * 8 + [dma((tp,))] * 2 + [dma((ep * tp,))] * 2
    shapes = (
        jax.ShapeDtypeStruct((1, col_width), BF16),
        jax.ShapeDtypeStruct((1, channels), F32),
        jax.ShapeDtypeStruct((1, past, channels), BF16),
    )
    made = pl.pallas_call(
        functools.partial(layer_kernel, ep, tp),
        out_shape=shapes,
        in_specs=[pl.BlockSpec(memory_space=pl.ANY)] * len(args),
        out_specs=[pl.BlockSpec(memory_space=pltpu.VMEM)] * 3,
        scratch_shapes=scratch,
        compiler_params=pltpu.CompilerParams(
            collective_id=0, has_side_effects=True, vmem_limit_bytes=60 * 1024 * 1024
        ),
    )(*args)
    return pl.pallas_call(
        hand_over,
        out_shape=shapes,
        in_specs=[pl.BlockSpec(memory_space=pltpu.VMEM)] * 3,
        out_specs=[pl.BlockSpec(memory_space=pltpu.VMEM)] * 3,
    )(*made)


def solution(mesh):
    placed = (
        P(("grp", "ep"), None),
        P(("grp", "ep"), None, "tp"),
        P(("grp", "ep"), "tp"),
        P(),
        P(),
        P("ep", "tp"),
        P("ep", "tp"),
        P(None, "tp"),
        P("tp", None, None),
        P("tp", None, None),
        P("tp"),
        P("tp", None),
        P("grp", None),
        P("grp", None),
        P("ep", None, "tp"),
        P("ep", None, "tp"),
        P("ep", "tp", None),
        P(),
        P(None, ("ep", "tp")),
        P(None, ("ep", "tp")),
        P(("ep", "tp"), None),
    )
    return jax.shard_map(
        functools.partial(on_device, mesh.shape["ep"], mesh.shape["tp"]),
        mesh=mesh,
        in_specs=placed,
        out_specs=(P(("grp", "ep"), "tp"), P(("grp", "ep"), "tp"), P(("grp", "ep"), None, "tp")),
        check_vma=False,
    )
```

```python
import functools

import jax
import jax.numpy as jnp
from jax import lax
from jax.experimental import pallas as pl
from jax.experimental.pallas import tpu as pltpu
from jax.sharding import PartitionSpec as P

MESH = pl.DeviceIdType.MESH
F32 = jnp.float32
BF16 = jnp.bfloat16


def each(count, step):
    if count <= 16:
        for number in range(count):
            step(number)
    else:

        def body(number, carry):
            step(number)
            return carry

        lax.fori_loop(0, count, body, 0)


def mm(left, right):
    return jnp.dot(left, right, preferred_element_type=F32)


def silu(value):
    return value * jax.nn.sigmoid(value)


def layer_kernel(
    ep,
    tp,
    tokens,
    conv_state,
    state_h,
    mixer_gain,
    expert_gain,
    input_proj,
    branch_proj,
    conv_taps,
    write_map,
    decay_map,
    decay_rate,
    output_proj,
    route_ids,
    route_scores,
    expert_gate,
    expert_up,
    expert_down,
    branch_gate,
    shared_gate,
    shared_up,
    shared_down,
    result_out,
    state_out,
    conv_out,
    tok_all,
    conv_all,
    state_all,
    mgain,
    egain,
    iproj,
    bproj,
    taps,
    wmap,
    dmap,
    rate,
    oproj,
    ids,
    scores,
    eg_w,
    eu_w,
    ed_w,
    bgate,
    sg_w,
    su_w,
    sd_w,
    norm_s,
    part_in,
    part_out,
    part_send,
    part_recv,
    resid_s,
    next_s,
    inner_s,
    local_sem,
    tok_ss,
    tok_rs,
    conv_ss,
    conv_rs,
    state_ss,
    state_rs,
    in_ss,
    in_rs,
    out_ss,
    out_rs,
    last_ss,
    last_rs,
):
    me_e = lax.axis_index("ep")
    me_t = lax.axis_index("tp")
    rows = ep
    width = tok_all.shape[-1]
    channels = iproj.shape[1]
    depth = iproj.shape[0]
    col_width = part_send.shape[-1]
    me_flat = me_e * tp + me_t

    small = [
        (tokens, tok_all.at[me_e]),
        (conv_state.at[0], conv_all.at[me_e]),
        (state_h, state_all.at[me_e]),
        (mixer_gain, mgain),
        (input_proj, iproj),
        (branch_proj, bproj),
        (conv_taps, taps),
        (write_map, wmap),
        (decay_map, dmap),
        (decay_rate, rate),
        (output_proj, oproj),
        (expert_gain, egain),
        (route_ids, ids),
        (route_scores, scores),
        (branch_gate, bgate),
    ]
    large = [
        (shared_gate, sg_w),
        (shared_up, su_w),
        (expert_gate.at[0], eg_w),
        (expert_up.at[0], eu_w),
        (expert_down.at[0], ed_w),
        (shared_down, sd_w),
    ]
    local = [
        pltpu.make_async_copy(src, dst, local_sem.at[number])
        for number, (src, dst) in enumerate(small + large)
    ]
    (
        c_tok,
        c_conv,
        c_state,
        c_mgain,
        c_iproj,
        c_bproj,
        c_taps,
        c_wmap,
        c_dmap,
        c_rate,
        c_oproj,
        c_egain,
        c_ids,
        c_scores,
        c_bgate,
        c_sg,
        c_su,
        c_eg,
        c_eu,
        c_ed,
        c_sd,
    ) = local
    for copy in local[: len(small)]:
        copy.start()

    barrier = pltpu.get_barrier_semaphore()

    def greet(peer):
        pl.semaphore_signal(barrier, inc=1, device_id=peer, device_id_type=MESH)

    each(ep - 1, lambda n: greet({"ep": lax.rem(me_e + 1 + n, ep)}))
    each(tp - 1, lambda n: greet({"tp": lax.rem(me_t + 1 + n, tp)}))
    c_mgain.wait()
    gain1 = mgain[...].astype(F32).reshape(1, width)
    norm_s[0:1] = gain1
    pl.semaphore_wait(barrier, ep + tp - 2)

    def over_ep(buf, ssem, rsem, slot, peer):
        return pltpu.make_async_remote_copy(
            src_ref=buf.at[slot],
            dst_ref=buf.at[slot],
            send_sem=ssem.at[peer],
            recv_sem=rsem.at[slot],
            device_id={"ep": peer},
            device_id_type=MESH,
        )

    def over_tp(buf, ssem, rsem, slot, peer):
        return pltpu.make_async_remote_copy(
            src_ref=buf.at[slot],
            dst_ref=buf.at[slot],
            send_sem=ssem.at[peer],
            recv_sem=rsem.at[slot],
            device_id={"tp": peer},
            device_id_type=MESH,
        )

    def ep_peer(number):
        return lax.rem(me_e + 1 + number, ep)

    def tp_peer(number):
        return lax.rem(me_t + 1 + number, tp)

    def send_ep(buf, ssem, rsem):
        each(ep - 1, lambda n: over_ep(buf, ssem, rsem, me_e, ep_peer(n)).start())

    def recv_ep(buf, ssem, rsem):
        each(ep - 1, lambda n: over_ep(buf, ssem, rsem, ep_peer(n), ep_peer(n)).wait_recv())

    def sent_ep(buf, ssem, rsem):
        each(ep - 1, lambda n: over_ep(buf, ssem, rsem, me_e, ep_peer(n)).wait_send())

    c_tok.wait()
    send_ep(tok_all, tok_ss, tok_rs)
    c_conv.wait()
    send_ep(conv_all, conv_ss, conv_rs)
    c_state.wait()
    send_ep(state_all, state_ss, state_rs)
    for copy in local[len(small) :]:
        copy.start()

    c_iproj.wait()
    c_bproj.wait()
    recv_ep(tok_all, tok_ss, tok_rs)
    if depth % 128 == 0:
        own_cols = pl.ds(pl.multiple_of(me_e * depth, depth), depth)
        mine = jnp.concatenate(
            [tok_all[row, :, own_cols].astype(F32) for row in range(rows)], axis=0
        )
        mine = mine * norm_s[0:1, own_cols]
    else:
        mine = jnp.concatenate([tok_all[row].astype(F32) for row in range(rows)], axis=0) * gain1
        mine = pltpu.roll(mine, lax.rem(width - me_e * depth, width), 1)[:, :depth]
    mine = mine.astype(BF16)
    part_in[me_e] = jnp.concatenate([mm(mine, iproj[...]), mm(mine, bproj[...])], axis=1).astype(
        BF16
    )
    send_ep(part_in, in_ss, in_rs)

    tok = jnp.concatenate([tok_all[row].astype(F32) for row in range(rows)], axis=0)
    scale = lax.rsqrt(jnp.mean(tok * tok, axis=-1, keepdims=True) + 1e-06)
    c_taps.wait()
    c_wmap.wait()
    c_dmap.wait()
    c_rate.wait()
    c_oproj.wait()
    recv_ep(conv_all, conv_ss, conv_rs)
    recv_ep(state_all, state_ss, state_rs)
    tap = taps[...].astype(F32)
    past = tap.shape[0] - 1
    history = jnp.concatenate(
        [
            jnp.sum(conv_all[row].astype(F32) * tap[:past], axis=0, keepdims=True)
            for row in range(rows)
        ],
        axis=0,
    )
    state = jnp.concatenate([state_all[row] for row in range(rows)], axis=0)
    rates = rate[...].reshape(1, channels)

    recv_ep(part_in, in_ss, in_rs)
    projected = jnp.sum(part_in[...].astype(F32), axis=0) * scale
    inner_x = projected[:, :channels].astype(BF16).astype(F32)
    branch_x = projected[:, channels:].astype(BF16).astype(F32)
    convolved = history + tap[past:] * inner_x
    conv_round = convolved.astype(BF16)
    heads, head_width = wmap.shape[0], wmap.shape[1]

    def by_head(maps):
        return jnp.concatenate(
            [
                mm(conv_round[:, h * head_width : (h + 1) * head_width], maps[h])
                for h in range(heads)
            ],
            axis=1,
        )

    write_gate = jax.nn.sigmoid(by_head(wmap))
    decay_gate = jax.nn.sigmoid(by_head(dmap))
    forget = 8.0 * decay_gate * rates
    bent = jnp.tanh(forget)
    state_next = (
        jnp.exp(-forget) * state
        + jnp.sqrt(2.0 * bent / (1.0 + bent)) * write_gate * convolved
    )
    mixed = (state_next * jax.nn.gelu(branch_x)).astype(BF16)
    part_out[me_t] = mm(mixed, oproj[...]).astype(BF16)
    each(tp - 1, lambda n: over_tp(part_out, out_ss, out_rs, me_t, tp_peer(n)).start())

    for row in range(rows):
        next_s[row] = state_next[row : row + 1]
        inner_s[row] = inner_x[row : row + 1]
    state_out[...] = next_s[me_e]
    conv_out[0] = jnp.concatenate([conv_all[me_e].astype(F32)[1:], inner_s[me_e]], axis=0).astype(
        BF16
    )
    c_egain.wait()
    c_ids.wait()
    c_scores.wait()
    c_bgate.wait()
    score = scores[...]
    share = score / jnp.sum(score, axis=0, keepdims=True)
    chosen = jnp.sum(jnp.where(ids[...] == me_e, share, 0.0), axis=0, keepdims=True)
    square = (rows, rows)
    diagonal = lax.broadcasted_iota(jnp.int32, square, 0) == lax.broadcasted_iota(
        jnp.int32, square, 1
    )
    chosen = jnp.sum(jnp.where(diagonal, chosen, 0.0), axis=1, keepdims=True)
    gain2 = egain[...].astype(F32).reshape(1, width)
    mixer = bgate[...].astype(F32).reshape(1, width)
    for copy in local[len(small) :]:
        copy.wait()

    each(tp - 1, lambda n: over_tp(part_out, out_ss, out_rs, tp_peer(n), tp_peer(n)).wait_recv())
    resid = (tok + jnp.sum(part_out[...].astype(F32), axis=0)).astype(BF16).astype(F32)
    scale2 = lax.rsqrt(jnp.mean(resid * resid, axis=-1, keepdims=True) + 1e-06)
    bare = resid * gain2
    blend = jax.nn.sigmoid(jnp.sum(bare * mixer, axis=-1, keepdims=True) * scale2)
    bare = bare.astype(BF16)
    dense = (silu(mm(bare, sg_w[...]) * scale2) * (mm(bare, su_w[...]) * scale2)).astype(BF16)
    hidden = (silu(mm(bare, eg_w[...]) * scale2) * (mm(bare, eu_w[...]) * scale2)).astype(BF16)

    def last(col, row, slot):
        return pltpu.make_async_remote_copy(
            src_ref=part_send.at[col, row],
            dst_ref=part_recv.at[slot],
            send_sem=last_ss.at[row * tp + col],
            recv_sem=last_rs.at[slot],
            device_id={"ep": row, "tp": col},
            device_id_type=MESH,
        )

    if tp % 2 == 0:
        turn = me_t + 1 - 2 * lax.rem(me_t, 2)
        order = [
            lax.rem(base + 2 * pair, tp) for pair in range(1, tp // 2) for base in (me_t, turn)
        ]
        order += [turn, me_t]
    else:
        order = [lax.rem(me_t + 1 + step, tp) for step in range(tp)]
    for step, col in enumerate(order):
        at = pl.ds(pl.multiple_of(col * col_width, col_width), col_width)
        sums = (chosen * mm(hidden, ed_w[:, at]) + blend * mm(dense, sd_w[:, at])).astype(BF16)
        for row in range(rows):
            part_send[col, row] = sums[row : row + 1]
        count = ep - 1 if step == tp - 1 else ep
        each(count, lambda n: last(col, ep_peer(n), me_flat).start())
    part_recv[me_flat] = part_send[me_t, me_e]
    for row in range(rows):
        resid_s[row] = resid[row : row + 1]
    own = resid_s[me_e, :, pl.ds(pl.multiple_of(me_t * col_width, col_width), col_width)]

    def other(number):
        flat = lax.rem(me_flat + 1 + number, ep * tp)
        return flat // tp, lax.rem(flat, tp), flat

    def recv_last(number):
        row, col, flat = other(number)
        last(col, row, flat).wait_recv()

    def sent_last(number):
        row, col, flat = other(number)
        last(col, row, flat).wait_send()

    each(ep * tp - 1, recv_last)
    total = own + jnp.sum(part_recv[...].astype(F32), axis=0)
    result_out[...] = total.astype(BF16)

    sent_ep(tok_all, tok_ss, tok_rs)
    sent_ep(conv_all, conv_ss, conv_rs)
    sent_ep(state_all, state_ss, state_rs)
    sent_ep(part_in, in_ss, in_rs)
    each(tp - 1, lambda n: over_tp(part_out, out_ss, out_rs, me_t, tp_peer(n)).wait_send())
    each(ep * tp - 1, sent_last)


def hand_over(result, state, conv, result_out, state_out, conv_out):
    result_out[...] = result[...]
    state_out[...] = state[...]
    conv_out[...] = conv[...]


def on_device(ep, tp, *args):
    (
        tokens,
        conv_state,
        state_h,
        mixer_gain,
        expert_gain,
        input_proj,
        branch_proj,
        conv_taps,
        write_map,
        decay_map,
        decay_rate,
        output_proj,
        route_ids,
        route_scores,
        expert_gate,
        expert_up,
        expert_down,
        branch_gate,
        shared_gate,
        shared_up,
        shared_down,
    ) = args
    assert tokens.shape[0] == 1
    route_ids, route_scores = route_ids.T, route_scores.T
    args = args[:12] + (route_ids, route_scores) + args[14:]
    rows = ep
    width = tokens.shape[1]
    channels = state_h.shape[1]
    col_width = width // tp
    past = conv_state.shape[1]

    def like(array):
        return pltpu.VMEM(array.shape, array.dtype)

    def inner(array):
        return pltpu.VMEM(array.shape[1:], array.dtype)

    dma = pltpu.SemaphoreType.DMA
    scratch = [
        pltpu.VMEM((rows, 1, width), BF16),
        pltpu.VMEM((rows, past, channels), BF16),
        pltpu.VMEM((rows, 1, channels), F32),
        like(mixer_gain),
        like(expert_gain),
        like(input_proj),
        like(branch_proj),
        like(conv_taps),
        like(write_map),
        like(decay_map),
        like(decay_rate),
        like(output_proj),
        like(route_ids),
        like(route_scores),
        inner(expert_gate),
        inner(expert_up),
        inner(expert_down),
        like(branch_gate),
        like(shared_gate),
        like(shared_up),
        like(shared_down),
        pltpu.VMEM((8, width), F32),
        pltpu.VMEM((ep, rows, 2 * channels), BF16),
        pltpu.VMEM((tp, rows, width), BF16),
        pltpu.VMEM((tp, rows, 1, col_width), BF16),
        pltpu.VMEM((ep * tp, 1, col_width), BF16),
        pltpu.VMEM((rows, 1, width), F32),
        pltpu.VMEM((rows, 1, channels), F32),
        pltpu.VMEM((rows, 1, channels), F32),
        dma((len(args),)),
    ]
    scratch += [dma((ep,))] * 8 + [dma((tp,))] * 2 + [dma((ep * tp,))] * 2
    shapes = (
        jax.ShapeDtypeStruct((1, col_width), BF16),
        jax.ShapeDtypeStruct((1, channels), F32),
        jax.ShapeDtypeStruct((1, past, channels), BF16),
    )
    made = pl.pallas_call(
        functools.partial(layer_kernel, ep, tp),
        out_shape=shapes,
        in_specs=[pl.BlockSpec(memory_space=pl.ANY)] * len(args),
        out_specs=[pl.BlockSpec(memory_space=pltpu.VMEM)] * 3,
        scratch_shapes=scratch,
        compiler_params=pltpu.CompilerParams(
            collective_id=0, has_side_effects=True, vmem_limit_bytes=60 * 1024 * 1024
        ),
    )(*args)
    return pl.pallas_call(
        hand_over,
        out_shape=shapes,
        in_specs=[pl.BlockSpec(memory_space=pltpu.VMEM)] * 3,
        out_specs=[pl.BlockSpec(memory_space=pltpu.VMEM)] * 3,
    )(*made)


def solution(mesh):
    placed = (
        P(("grp", "ep"), None),
        P(("grp", "ep"), None, "tp"),
        P(("grp", "ep"), "tp"),
        P(),
        P(),
        P("ep", "tp"),
        P("ep", "tp"),
        P(None, "tp"),
        P("tp", None, None),
        P("tp", None, None),
        P("tp"),
        P("tp", None),
        P("grp", None),
        P("grp", None),
        P("ep", None, "tp"),
        P("ep", None, "tp"),
        P("ep", "tp", None),
        P(),
        P(None, ("ep", "tp")),
        P(None, ("ep", "tp")),
        P(("ep", "tp"), None),
    )
    return jax.shard_map(
        functools.partial(on_device, mesh.shape["ep"], mesh.shape["tp"]),
        mesh=mesh,
        in_specs=placed,
        out_specs=(P(("grp", "ep"), "tp"), P(("grp", "ep"), "tp"), P(("grp", "ep"), None, "tp")),
        check_vma=False,
    )
```

```python
import functools

import jax
import jax.numpy as jnp
from jax import lax
from jax.experimental import pallas as pl
from jax.experimental.pallas import tpu as pltpu
from jax.sharding import PartitionSpec as P

MESH = pl.DeviceIdType.MESH
F32 = jnp.float32
BF16 = jnp.bfloat16


def each(count, step):
    if count <= 16:
        for number in range(count):
            step(number)
    else:

        def body(number, carry):
            step(number)
            return carry

        lax.fori_loop(0, count, body, 0)


def mm(left, right):
    return jnp.dot(left, right, preferred_element_type=F32)


def silu(value):
    return value * jax.nn.sigmoid(value)


def layer_kernel(
    ep,
    tp,
    tokens,
    conv_state,
    state_h,
    mixer_gain,
    expert_gain,
    input_proj,
    branch_proj,
    conv_taps,
    write_map,
    decay_map,
    decay_rate,
    output_proj,
    route_ids,
    route_scores,
    expert_gate,
    expert_up,
    expert_down,
    branch_gate,
    shared_gate,
    shared_up,
    shared_down,
    part_recv,
    own_out,
    state_out,
    conv_out,
    tok_all,
    conv_all,
    state_all,
    mgain,
    egain,
    iproj,
    bproj,
    taps,
    wmap,
    dmap,
    rate,
    oproj,
    ids,
    scores,
    eg_w,
    eu_w,
    ed_w,
    bgate,
    sg_w,
    su_w,
    sd_w,
    norm_s,
    part_in,
    part_out,
    part_send,
    resid_s,
    next_s,
    inner_s,
    conv_s,
    out_sem,
    local_sem,
    tok_ss,
    tok_rs,
    conv_ss,
    conv_rs,
    state_ss,
    state_rs,
    in_ss,
    in_rs,
    out_ss,
    out_rs,
    last_ss,
    last_rs,
):
    me_e = lax.axis_index("ep")
    me_t = lax.axis_index("tp")
    rows = ep
    width = tok_all.shape[-1]
    channels = iproj.shape[1]
    depth = iproj.shape[0]
    col_width = part_send.shape[-1]
    me_flat = me_e * tp + me_t

    small = [
        (tokens, tok_all.at[me_e]),
        (conv_state.at[0], conv_all.at[me_e]),
        (state_h, state_all.at[me_e]),
        (mixer_gain, mgain),
        (input_proj, iproj),
        (branch_proj, bproj),
        (conv_taps, taps),
        (write_map, wmap),
        (decay_map, dmap),
        (decay_rate, rate),
        (output_proj, oproj),
        (expert_gain, egain),
        (route_ids, ids),
        (route_scores, scores),
        (branch_gate, bgate),
    ]
    large = [
        (shared_gate, sg_w),
        (shared_up, su_w),
        (expert_gate.at[0], eg_w),
        (expert_up.at[0], eu_w),
        (expert_down.at[0], ed_w),
        (shared_down, sd_w),
    ]
    local = [
        pltpu.make_async_copy(src, dst, local_sem.at[number])
        for number, (src, dst) in enumerate(small + large)
    ]
    (
        c_tok,
        c_conv,
        c_state,
        c_mgain,
        c_iproj,
        c_bproj,
        c_taps,
        c_wmap,
        c_dmap,
        c_rate,
        c_oproj,
        c_egain,
        c_ids,
        c_scores,
        c_bgate,
        c_sg,
        c_su,
        c_eg,
        c_eu,
        c_ed,
        c_sd,
    ) = local
    for copy in local[: len(small)]:
        copy.start()

    barrier = pltpu.get_barrier_semaphore()

    def greet(peer):
        pl.semaphore_signal(barrier, inc=1, device_id=peer, device_id_type=MESH)

    each(ep - 1, lambda n: greet({"ep": lax.rem(me_e + 1 + n, ep)}))
    each(tp - 1, lambda n: greet({"tp": lax.rem(me_t + 1 + n, tp)}))
    c_mgain.wait()
    gain1 = mgain[...].astype(F32).reshape(1, width)
    norm_s[0:1] = gain1
    pl.semaphore_wait(barrier, ep + tp - 2)

    def over_ep(buf, ssem, rsem, slot, peer):
        return pltpu.make_async_remote_copy(
            src_ref=buf.at[slot],
            dst_ref=buf.at[slot],
            send_sem=ssem.at[peer],
            recv_sem=rsem.at[slot],
            device_id={"ep": peer},
            device_id_type=MESH,
        )

    def over_tp(buf, ssem, rsem, slot, peer):
        return pltpu.make_async_remote_copy(
            src_ref=buf.at[slot],
            dst_ref=buf.at[slot],
            send_sem=ssem.at[peer],
            recv_sem=rsem.at[slot],
            device_id={"tp": peer},
            device_id_type=MESH,
        )

    def ep_peer(number):
        return lax.rem(me_e + 1 + number, ep)

    def tp_peer(number):
        return lax.rem(me_t + 1 + number, tp)

    def send_ep(buf, ssem, rsem):
        each(ep - 1, lambda n: over_ep(buf, ssem, rsem, me_e, ep_peer(n)).start())

    def recv_ep(buf, ssem, rsem):
        each(ep - 1, lambda n: over_ep(buf, ssem, rsem, ep_peer(n), ep_peer(n)).wait_recv())

    def sent_ep(buf, ssem, rsem):
        each(ep - 1, lambda n: over_ep(buf, ssem, rsem, me_e, ep_peer(n)).wait_send())

    c_tok.wait()
    send_ep(tok_all, tok_ss, tok_rs)
    c_conv.wait()
    send_ep(conv_all, conv_ss, conv_rs)
    c_state.wait()
    send_ep(state_all, state_ss, state_rs)
    for copy in local[len(small) :]:
        copy.start()

    c_iproj.wait()
    c_bproj.wait()
    recv_ep(tok_all, tok_ss, tok_rs)
    if depth % 128 == 0:
        own_cols = pl.ds(pl.multiple_of(me_e * depth, depth), depth)
        mine = jnp.concatenate(
            [tok_all[row, :, own_cols].astype(F32) for row in range(rows)], axis=0
        )
        mine = mine * norm_s[0:1, own_cols]
    else:
        mine = jnp.concatenate([tok_all[row].astype(F32) for row in range(rows)], axis=0) * gain1
        mine = pltpu.roll(mine, lax.rem(width - me_e * depth, width), 1)[:, :depth]
    mine = mine.astype(BF16)
    part_in[me_e] = jnp.concatenate([mm(mine, iproj[...]), mm(mine, bproj[...])], axis=1).astype(
        BF16
    )
    send_ep(part_in, in_ss, in_rs)

    tok = jnp.concatenate([tok_all[row].astype(F32) for row in range(rows)], axis=0)
    scale = lax.rsqrt(jnp.mean(tok * tok, axis=-1, keepdims=True) + 1e-06)
    c_taps.wait()
    c_wmap.wait()
    c_dmap.wait()
    c_rate.wait()
    c_oproj.wait()
    recv_ep(conv_all, conv_ss, conv_rs)
    recv_ep(state_all, state_ss, state_rs)
    tap = taps[...].astype(F32)
    past = tap.shape[0] - 1
    history = jnp.concatenate(
        [
            jnp.sum(conv_all[row].astype(F32) * tap[:past], axis=0, keepdims=True)
            for row in range(rows)
        ],
        axis=0,
    )
    state = jnp.concatenate([state_all[row] for row in range(rows)], axis=0)
    rates = rate[...].reshape(1, channels)

    recv_ep(part_in, in_ss, in_rs)
    projected = jnp.sum(part_in[...].astype(F32), axis=0) * scale
    inner_x = projected[:, :channels].astype(BF16).astype(F32)
    branch_x = projected[:, channels:].astype(BF16).astype(F32)
    convolved = history + tap[past:] * inner_x
    conv_round = convolved.astype(BF16)
    heads, head_width = wmap.shape[0], wmap.shape[1]

    def by_head(maps):
        return jnp.concatenate(
            [
                mm(conv_round[:, h * head_width : (h + 1) * head_width], maps[h])
                for h in range(heads)
            ],
            axis=1,
        )

    write_gate = jax.nn.sigmoid(by_head(wmap))
    decay_gate = jax.nn.sigmoid(by_head(dmap))
    forget = 8.0 * decay_gate * rates
    bent = jnp.tanh(forget)
    state_next = (
        jnp.exp(-forget) * state
        + jnp.sqrt(2.0 * bent / (1.0 + bent)) * write_gate * convolved
    )
    mixed = (state_next * jax.nn.gelu(branch_x)).astype(BF16)
    part_out[me_t] = mm(mixed, oproj[...]).astype(BF16)
    each(tp - 1, lambda n: over_tp(part_out, out_ss, out_rs, me_t, tp_peer(n)).start())

    for row in range(rows):
        next_s[row] = state_next[row : row + 1]
        inner_s[row] = inner_x[row : row + 1]
    c_next = pltpu.make_async_copy(next_s.at[me_e], state_out, out_sem.at[0])
    c_next.start()
    conv_s[0] = jnp.concatenate([conv_all[me_e].astype(F32)[1:], inner_s[me_e]], axis=0).astype(
        BF16
    )
    c_past = pltpu.make_async_copy(conv_s, conv_out, out_sem.at[1])
    c_past.start()
    c_egain.wait()
    c_ids.wait()
    c_scores.wait()
    c_bgate.wait()
    score = scores[...]
    share = score / jnp.sum(score, axis=0, keepdims=True)
    chosen = jnp.sum(jnp.where(ids[...] == me_e, share, 0.0), axis=0, keepdims=True)
    square = (rows, rows)
    diagonal = lax.broadcasted_iota(jnp.int32, square, 0) == lax.broadcasted_iota(
        jnp.int32, square, 1
    )
    chosen = jnp.sum(jnp.where(diagonal, chosen, 0.0), axis=1, keepdims=True)
    gain2 = egain[...].astype(F32).reshape(1, width)
    mixer = bgate[...].astype(F32).reshape(1, width)
    for copy in local[len(small) :]:
        copy.wait()

    each(tp - 1, lambda n: over_tp(part_out, out_ss, out_rs, tp_peer(n), tp_peer(n)).wait_recv())
    resid = (tok + jnp.sum(part_out[...].astype(F32), axis=0)).astype(BF16).astype(F32)
    scale2 = lax.rsqrt(jnp.mean(resid * resid, axis=-1, keepdims=True) + 1e-06)
    bare = resid * gain2
    blend = jax.nn.sigmoid(jnp.sum(bare * mixer, axis=-1, keepdims=True) * scale2)
    bare = bare.astype(BF16)
    dense = (silu(mm(bare, sg_w[...]) * scale2) * (mm(bare, su_w[...]) * scale2)).astype(BF16)
    hidden = (silu(mm(bare, eg_w[...]) * scale2) * (mm(bare, eu_w[...]) * scale2)).astype(BF16)

    def last(col, row, slot):
        return pltpu.make_async_remote_copy(
            src_ref=part_send.at[col, row],
            dst_ref=part_recv.at[slot],
            send_sem=last_ss.at[row * tp + col],
            recv_sem=last_rs.at[slot],
            device_id={"ep": row, "tp": col},
            device_id_type=MESH,
        )

    if tp % 2 == 0:
        turn = me_t + 1 - 2 * lax.rem(me_t, 2)
        order = [
            lax.rem(base + 2 * pair, tp) for pair in range(1, tp // 2) for base in (me_t, turn)
        ]
        order += [turn, me_t]
    else:
        order = [lax.rem(me_t + 1 + step, tp) for step in range(tp)]
    for step, col in enumerate(order):
        at = pl.ds(pl.multiple_of(col * col_width, col_width), col_width)
        sums = (chosen * mm(hidden, ed_w[:, at]) + blend * mm(dense, sd_w[:, at])).astype(BF16)
        for row in range(rows):
            part_send[col, row] = sums[row : row + 1]
        count = ep - 1 if step == tp - 1 else ep
        each(count, lambda n: last(col, ep_peer(n), me_flat).start())
    c_part = pltpu.make_async_copy(
        part_send.at[me_t, me_e], part_recv.at[me_flat], out_sem.at[2]
    )
    c_part.start()
    for row in range(rows):
        resid_s[row] = resid[row : row + 1]
    c_own = pltpu.make_async_copy(
        resid_s.at[me_e, :, pl.ds(pl.multiple_of(me_t * col_width, col_width), col_width)],
        own_out,
        out_sem.at[3],
    )
    c_own.start()

    def other(number):
        flat = lax.rem(me_flat + 1 + number, ep * tp)
        return flat // tp, lax.rem(flat, tp), flat

    def recv_last(number):
        row, col, flat = other(number)
        last(col, row, flat).wait_recv()

    def sent_last(number):
        row, col, flat = other(number)
        last(col, row, flat).wait_send()

    sent_ep(tok_all, tok_ss, tok_rs)
    sent_ep(conv_all, conv_ss, conv_rs)
    sent_ep(state_all, state_ss, state_rs)
    sent_ep(part_in, in_ss, in_rs)
    each(tp - 1, lambda n: over_tp(part_out, out_ss, out_rs, me_t, tp_peer(n)).wait_send())
    each(ep * tp - 1, sent_last)
    for copy in (c_next, c_past, c_part, c_own):
        copy.wait()
    each(ep * tp - 1, recv_last)


def hand_over(parts, own, state, conv, result_out, state_out, conv_out):
    result_out[...] = (own[...] + jnp.sum(parts[...].astype(F32), axis=0)).astype(BF16)
    state_out[...] = state[...]
    conv_out[...] = conv[...]


def on_device(ep, tp, *args):
    (
        tokens,
        conv_state,
        state_h,
        mixer_gain,
        expert_gain,
        input_proj,
        branch_proj,
        conv_taps,
        write_map,
        decay_map,
        decay_rate,
        output_proj,
        route_ids,
        route_scores,
        expert_gate,
        expert_up,
        expert_down,
        branch_gate,
        shared_gate,
        shared_up,
        shared_down,
    ) = args
    assert tokens.shape[0] == 1
    route_ids, route_scores = route_ids.T, route_scores.T
    args = args[:12] + (route_ids, route_scores) + args[14:]
    rows = ep
    width = tokens.shape[1]
    channels = state_h.shape[1]
    col_width = width // tp
    past = conv_state.shape[1]

    def like(array):
        return pltpu.VMEM(array.shape, array.dtype)

    def inner(array):
        return pltpu.VMEM(array.shape[1:], array.dtype)

    dma = pltpu.SemaphoreType.DMA
    scratch = [
        pltpu.VMEM((rows, 1, width), BF16),
        pltpu.VMEM((rows, past, channels), BF16),
        pltpu.VMEM((rows, 1, channels), F32),
        like(mixer_gain),
        like(expert_gain),
        like(input_proj),
        like(branch_proj),
        like(conv_taps),
        like(write_map),
        like(decay_map),
        like(decay_rate),
        like(output_proj),
        like(route_ids),
        like(route_scores),
        inner(expert_gate),
        inner(expert_up),
        inner(expert_down),
        like(branch_gate),
        like(shared_gate),
        like(shared_up),
        like(shared_down),
        pltpu.VMEM((8, width), F32),
        pltpu.VMEM((ep, rows, 2 * channels), BF16),
        pltpu.VMEM((tp, rows, width), BF16),
        pltpu.VMEM((tp, rows, 1, col_width), BF16),
        pltpu.VMEM((rows, 1, width), F32),
        pltpu.VMEM((rows, 1, channels), F32),
        pltpu.VMEM((rows, 1, channels), F32),
        pltpu.VMEM((1, past, channels), BF16),
        dma((4,)),
        dma((len(args),)),
    ]
    scratch += [dma((ep,))] * 8 + [dma((tp,))] * 2 + [dma((ep * tp,))] * 2
    shapes = (
        jax.ShapeDtypeStruct((1, col_width), BF16),
        jax.ShapeDtypeStruct((1, channels), F32),
        jax.ShapeDtypeStruct((1, past, channels), BF16),
    )
    made = pl.pallas_call(
        functools.partial(layer_kernel, ep, tp),
        out_shape=(
            jax.ShapeDtypeStruct((ep * tp, 1, col_width), BF16),
            jax.ShapeDtypeStruct((1, col_width), F32),
        )
        + shapes[1:],
        in_specs=[pl.BlockSpec(memory_space=pl.ANY)] * len(args),
        out_specs=[pl.BlockSpec(memory_space=pl.ANY)] * 4,
        scratch_shapes=scratch,
        compiler_params=pltpu.CompilerParams(
            collective_id=0, has_side_effects=True, vmem_limit_bytes=60 * 1024 * 1024
        ),
    )(*args)
    return pl.pallas_call(
        hand_over,
        out_shape=shapes,
        in_specs=[pl.BlockSpec(memory_space=pltpu.VMEM)] * 4,
        out_specs=[pl.BlockSpec(memory_space=pltpu.VMEM)] * 3,
    )(*made)


def solution(mesh):
    placed = (
        P(("grp", "ep"), None),
        P(("grp", "ep"), None, "tp"),
        P(("grp", "ep"), "tp"),
        P(),
        P(),
        P("ep", "tp"),
        P("ep", "tp"),
        P(None, "tp"),
        P("tp", None, None),
        P("tp", None, None),
        P("tp"),
        P("tp", None),
        P("grp", None),
        P("grp", None),
        P("ep", None, "tp"),
        P("ep", None, "tp"),
        P("ep", "tp", None),
        P(),
        P(None, ("ep", "tp")),
        P(None, ("ep", "tp")),
        P(("ep", "tp"), None),
    )
    return jax.shard_map(
        functools.partial(on_device, mesh.shape["ep"], mesh.shape["tp"]),
        mesh=mesh,
        in_specs=placed,
        out_specs=(P(("grp", "ep"), "tp"), P(("grp", "ep"), "tp"), P(("grp", "ep"), None, "tp")),
        check_vma=False,
    )
```

```python
import functools

import jax
import jax.numpy as jnp
from jax import lax
from jax.experimental import pallas as pl
from jax.experimental.pallas import tpu as pltpu
from jax.sharding import PartitionSpec as P

MESH = pl.DeviceIdType.MESH
F32 = jnp.float32
BF16 = jnp.bfloat16


def each(count, step):
    if count <= 16:
        for number in range(count):
            step(number)
    else:

        def body(number, carry):
            step(number)
            return carry

        lax.fori_loop(0, count, body, 0)


def mm(left, right):
    return jnp.dot(left, right, preferred_element_type=F32)


def silu(value):
    return value * jax.nn.sigmoid(value)


def layer_kernel(
    ep,
    tp,
    tokens,
    conv_state,
    state_h,
    mixer_gain,
    expert_gain,
    input_proj,
    branch_proj,
    conv_taps,
    write_map,
    decay_map,
    decay_rate,
    output_proj,
    route_ids,
    route_scores,
    expert_gate,
    expert_up,
    expert_down,
    branch_gate,
    shared_gate,
    shared_up,
    shared_down,
    part_recv,
    own_out,
    state_out,
    conv_out,
    tok_all,
    conv_all,
    state_all,
    mgain,
    egain,
    iproj,
    bproj,
    taps,
    wmap,
    dmap,
    rate,
    oproj,
    ids,
    scores,
    eg_w,
    eu_w,
    ed_w,
    bgate,
    sg_w,
    su_w,
    sd_w,
    norm_s,
    part_in,
    part_out,
    part_send,
    resid_s,
    next_s,
    inner_s,
    conv_s,
    out_sem,
    local_sem,
    tok_ss,
    tok_rs,
    conv_ss,
    conv_rs,
    state_ss,
    state_rs,
    in_ss,
    in_rs,
    out_ss,
    out_rs,
    last_ss,
    last_rs,
):
    me_e = lax.axis_index("ep")
    me_t = lax.axis_index("tp")
    rows = ep
    width = tok_all.shape[-1]
    channels = iproj.shape[1]
    depth = iproj.shape[0]
    col_width = part_send.shape[-1]
    me_flat = me_e * tp + me_t

    small = [
        (tokens, tok_all.at[me_e]),
        (conv_state.at[0], conv_all.at[me_e]),
        (state_h, state_all.at[me_e]),
        (mixer_gain, mgain),
        (input_proj, iproj),
        (branch_proj, bproj),
        (conv_taps, taps),
        (write_map, wmap),
        (decay_map, dmap),
        (decay_rate, rate),
        (output_proj, oproj),
        (expert_gain, egain),
        (route_ids, ids),
        (route_scores, scores),
        (branch_gate, bgate),
    ]
    large = [
        (shared_gate, sg_w),
        (shared_up, su_w),
        (expert_gate.at[0], eg_w),
        (expert_up.at[0], eu_w),
        (expert_down.at[0], ed_w),
        (shared_down, sd_w),
    ]
    local = [
        pltpu.make_async_copy(src, dst, local_sem.at[number])
        for number, (src, dst) in enumerate(small + large)
    ]
    (
        c_tok,
        c_conv,
        c_state,
        c_mgain,
        c_iproj,
        c_bproj,
        c_taps,
        c_wmap,
        c_dmap,
        c_rate,
        c_oproj,
        c_egain,
        c_ids,
        c_scores,
        c_bgate,
        c_sg,
        c_su,
        c_eg,
        c_eu,
        c_ed,
        c_sd,
    ) = local
    for copy in local[: len(small)]:
        copy.start()

    barrier = pltpu.get_barrier_semaphore()

    def greet(peer):
        pl.semaphore_signal(barrier, inc=1, device_id=peer, device_id_type=MESH)

    each(ep - 1, lambda n: greet({"ep": lax.rem(me_e + 1 + n, ep)}))
    each(tp - 1, lambda n: greet({"tp": lax.rem(me_t + 1 + n, tp)}))
    c_mgain.wait()
    gain1 = mgain[...].astype(F32).reshape(1, width)
    norm_s[0:1] = gain1
    pl.semaphore_wait(barrier, ep + tp - 2)

    def over_ep(buf, ssem, rsem, slot, peer):
        return pltpu.make_async_remote_copy(
            src_ref=buf.at[slot],
            dst_ref=buf.at[slot],
            send_sem=ssem.at[peer],
            recv_sem=rsem.at[slot],
            device_id={"ep": peer},
            device_id_type=MESH,
        )

    def over_tp(buf, ssem, rsem, slot, peer):
        return pltpu.make_async_remote_copy(
            src_ref=buf.at[slot],
            dst_ref=buf.at[slot],
            send_sem=ssem.at[peer],
            recv_sem=rsem.at[slot],
            device_id={"tp": peer},
            device_id_type=MESH,
        )

    def ep_peer(number):
        return lax.rem(me_e + 1 + number, ep)

    def far_peer(number):
        return lax.rem(me_e + 1 + (number + ep // 2 - 1) % (ep - 1), ep)

    def tp_peer(number):
        return lax.rem(me_t + 1 + number, tp)

    def send_ep(buf, ssem, rsem):
        each(ep - 1, lambda n: over_ep(buf, ssem, rsem, me_e, far_peer(n)).start())

    def recv_ep(buf, ssem, rsem):
        each(ep - 1, lambda n: over_ep(buf, ssem, rsem, ep_peer(n), ep_peer(n)).wait_recv())

    def sent_ep(buf, ssem, rsem):
        each(ep - 1, lambda n: over_ep(buf, ssem, rsem, me_e, ep_peer(n)).wait_send())

    c_tok.wait()
    send_ep(tok_all, tok_ss, tok_rs)
    c_conv.wait()
    send_ep(conv_all, conv_ss, conv_rs)
    c_state.wait()
    send_ep(state_all, state_ss, state_rs)
    for copy in local[len(small) :]:
        copy.start()

    c_iproj.wait()
    c_bproj.wait()
    recv_ep(tok_all, tok_ss, tok_rs)
    if depth % 128 == 0:
        own_cols = pl.ds(pl.multiple_of(me_e * depth, depth), depth)
        mine = jnp.concatenate(
            [tok_all[row, :, own_cols].astype(F32) for row in range(rows)], axis=0
        )
        mine = mine * norm_s[0:1, own_cols]
    else:
        mine = jnp.concatenate([tok_all[row].astype(F32) for row in range(rows)], axis=0) * gain1
        mine = pltpu.roll(mine, lax.rem(width - me_e * depth, width), 1)[:, :depth]
    mine = mine.astype(BF16)
    part_in[me_e] = jnp.concatenate([mm(mine, iproj[...]), mm(mine, bproj[...])], axis=1).astype(
        BF16
    )
    send_ep(part_in, in_ss, in_rs)

    tok = jnp.concatenate([tok_all[row].astype(F32) for row in range(rows)], axis=0)
    scale = lax.rsqrt(jnp.mean(tok * tok, axis=-1, keepdims=True) + 1e-06)
    c_taps.wait()
    c_wmap.wait()
    c_dmap.wait()
    c_rate.wait()
    c_oproj.wait()
    recv_ep(conv_all, conv_ss, conv_rs)
    recv_ep(state_all, state_ss, state_rs)
    tap = taps[...].astype(F32)
    past = tap.shape[0] - 1
    history = jnp.concatenate(
        [
            jnp.sum(conv_all[row].astype(F32) * tap[:past], axis=0, keepdims=True)
            for row in range(rows)
        ],
        axis=0,
    )
    state = jnp.concatenate([state_all[row] for row in range(rows)], axis=0)
    rates = rate[...].reshape(1, channels)

    recv_ep(part_in, in_ss, in_rs)
    projected = jnp.sum(part_in[...].astype(F32), axis=0) * scale
    inner_x = projected[:, :channels].astype(BF16).astype(F32)
    branch_x = projected[:, channels:].astype(BF16).astype(F32)
    convolved = history + tap[past:] * inner_x
    conv_round = convolved.astype(BF16)
    heads, head_width = wmap.shape[0], wmap.shape[1]

    def by_head(maps):
        return jnp.concatenate(
            [
                mm(conv_round[:, h * head_width : (h + 1) * head_width], maps[h])
                for h in range(heads)
            ],
            axis=1,
        )

    write_gate = jax.nn.sigmoid(by_head(wmap))
    decay_gate = jax.nn.sigmoid(by_head(dmap))
    forget = 8.0 * decay_gate * rates
    bent = jnp.tanh(forget)
    state_next = (
        jnp.exp(-forget) * state
        + jnp.sqrt(2.0 * bent / (1.0 + bent)) * write_gate * convolved
    )
    mixed = (state_next * jax.nn.gelu(branch_x)).astype(BF16)
    part_out[me_t] = mm(mixed, oproj[...]).astype(BF16)
    each(tp - 1, lambda n: over_tp(part_out, out_ss, out_rs, me_t, tp_peer(n)).start())

    for row in range(rows):
        next_s[row] = state_next[row : row + 1]
        inner_s[row] = inner_x[row : row + 1]
    c_next = pltpu.make_async_copy(next_s.at[me_e], state_out, out_sem.at[0])
    c_next.start()
    conv_s[0] = jnp.concatenate([conv_all[me_e].astype(F32)[1:], inner_s[me_e]], axis=0).astype(
        BF16
    )
    c_past = pltpu.make_async_copy(conv_s, conv_out, out_sem.at[1])
    c_past.start()
    c_egain.wait()
    c_ids.wait()
    c_scores.wait()
    c_bgate.wait()
    score = scores[...]
    share = score / jnp.sum(score, axis=0, keepdims=True)
    chosen = jnp.sum(jnp.where(ids[...] == me_e, share, 0.0), axis=0, keepdims=True)
    square = (rows, rows)
    diagonal = lax.broadcasted_iota(jnp.int32, square, 0) == lax.broadcasted_iota(
        jnp.int32, square, 1
    )
    chosen = jnp.sum(jnp.where(diagonal, chosen, 0.0), axis=1, keepdims=True)
    gain2 = egain[...].astype(F32).reshape(1, width)
    mixer = bgate[...].astype(F32).reshape(1, width)
    for copy in local[len(small) :]:
        copy.wait()

    each(tp - 1, lambda n: over_tp(part_out, out_ss, out_rs, tp_peer(n), tp_peer(n)).wait_recv())
    resid = (tok + jnp.sum(part_out[...].astype(F32), axis=0)).astype(BF16).astype(F32)
    scale2 = lax.rsqrt(jnp.mean(resid * resid, axis=-1, keepdims=True) + 1e-06)
    bare = resid * gain2
    blend = jax.nn.sigmoid(jnp.sum(bare * mixer, axis=-1, keepdims=True) * scale2)
    bare = bare.astype(BF16)
    dense = (silu(mm(bare, sg_w[...]) * scale2) * (mm(bare, su_w[...]) * scale2)).astype(BF16)
    hidden = (silu(mm(bare, eg_w[...]) * scale2) * (mm(bare, eu_w[...]) * scale2)).astype(BF16)

    def last(col, row, slot):
        return pltpu.make_async_remote_copy(
            src_ref=part_send.at[col, row],
            dst_ref=part_recv.at[slot],
            send_sem=last_ss.at[row * tp + col],
            recv_sem=last_rs.at[slot],
            device_id={"ep": row, "tp": col},
            device_id_type=MESH,
        )

    if tp % 2 == 0:
        turn = me_t + 1 - 2 * lax.rem(me_t, 2)
        order = [
            lax.rem(base + 2 * pair, tp) for pair in range(1, tp // 2) for base in (me_t, turn)
        ]
        order += [turn, me_t]
    else:
        order = [lax.rem(me_t + 1 + step, tp) for step in range(tp)]
    for step, col in enumerate(order):
        at = pl.ds(pl.multiple_of(col * col_width, col_width), col_width)
        sums = (chosen * mm(hidden, ed_w[:, at]) + blend * mm(dense, sd_w[:, at])).astype(BF16)
        for row in range(rows):
            part_send[col, row] = sums[row : row + 1]
        each(ep - 1, lambda n: last(col, far_peer(n), me_flat).start())
        if step < tp - 1:
            last(col, me_e, me_flat).start()
    c_part = pltpu.make_async_copy(
        part_send.at[me_t, me_e], part_recv.at[me_flat], out_sem.at[2]
    )
    c_part.start()
    for row in range(rows):
        resid_s[row] = resid[row : row + 1]
    c_own = pltpu.make_async_copy(
        resid_s.at[me_e, :, pl.ds(pl.multiple_of(me_t * col_width, col_width), col_width)],
        own_out,
        out_sem.at[3],
    )
    c_own.start()

    def other(number):
        flat = lax.rem(me_flat + 1 + number, ep * tp)
        return flat // tp, lax.rem(flat, tp), flat

    def recv_last(number):
        row, col, flat = other(number)
        last(col, row, flat).wait_recv()

    def sent_last(number):
        row, col, flat = other(number)
        last(col, row, flat).wait_send()

    sent_ep(tok_all, tok_ss, tok_rs)
    sent_ep(conv_all, conv_ss, conv_rs)
    sent_ep(state_all, state_ss, state_rs)
    sent_ep(part_in, in_ss, in_rs)
    each(tp - 1, lambda n: over_tp(part_out, out_ss, out_rs, me_t, tp_peer(n)).wait_send())
    each(ep * tp - 1, sent_last)
    for copy in (c_next, c_past, c_part, c_own):
        copy.wait()
    each(ep * tp - 1, recv_last)


def hand_over(parts, own, state, conv, result_out, state_out, conv_out):
    result_out[...] = (own[...] + jnp.sum(parts[...].astype(F32), axis=0)).astype(BF16)
    state_out[...] = state[...]
    conv_out[...] = conv[...]


def on_device(ep, tp, *args):
    (
        tokens,
        conv_state,
        state_h,
        mixer_gain,
        expert_gain,
        input_proj,
        branch_proj,
        conv_taps,
        write_map,
        decay_map,
        decay_rate,
        output_proj,
        route_ids,
        route_scores,
        expert_gate,
        expert_up,
        expert_down,
        branch_gate,
        shared_gate,
        shared_up,
        shared_down,
    ) = args
    assert tokens.shape[0] == 1
    route_ids, route_scores = route_ids.T, route_scores.T
    args = args[:12] + (route_ids, route_scores) + args[14:]
    rows = ep
    width = tokens.shape[1]
    channels = state_h.shape[1]
    col_width = width // tp
    past = conv_state.shape[1]

    def like(array):
        return pltpu.VMEM(array.shape, array.dtype)

    def inner(array):
        return pltpu.VMEM(array.shape[1:], array.dtype)

    dma = pltpu.SemaphoreType.DMA
    scratch = [
        pltpu.VMEM((rows, 1, width), BF16),
        pltpu.VMEM((rows, past, channels), BF16),
        pltpu.VMEM((rows, 1, channels), F32),
        like(mixer_gain),
        like(expert_gain),
        like(input_proj),
        like(branch_proj),
        like(conv_taps),
        like(write_map),
        like(decay_map),
        like(decay_rate),
        like(output_proj),
        like(route_ids),
        like(route_scores),
        inner(expert_gate),
        inner(expert_up),
        inner(expert_down),
        like(branch_gate),
        like(shared_gate),
        like(shared_up),
        like(shared_down),
        pltpu.VMEM((8, width), F32),
        pltpu.VMEM((ep, rows, 2 * channels), BF16),
        pltpu.VMEM((tp, rows, width), BF16),
        pltpu.VMEM((tp, rows, 1, col_width), BF16),
        pltpu.VMEM((rows, 1, width), F32),
        pltpu.VMEM((rows, 1, channels), F32),
        pltpu.VMEM((rows, 1, channels), F32),
        pltpu.VMEM((1, past, channels), BF16),
        dma((4,)),
        dma((len(args),)),
    ]
    scratch += [dma((ep,))] * 8 + [dma((tp,))] * 2 + [dma((ep * tp,))] * 2
    shapes = (
        jax.ShapeDtypeStruct((1, col_width), BF16),
        jax.ShapeDtypeStruct((1, channels), F32),
        jax.ShapeDtypeStruct((1, past, channels), BF16),
    )
    made = pl.pallas_call(
        functools.partial(layer_kernel, ep, tp),
        out_shape=(
            jax.ShapeDtypeStruct((ep * tp, 1, col_width), BF16),
            jax.ShapeDtypeStruct((1, col_width), F32),
        )
        + shapes[1:],
        in_specs=[pl.BlockSpec(memory_space=pl.ANY)] * len(args),
        out_specs=[pl.BlockSpec(memory_space=pl.ANY)] * 4,
        scratch_shapes=scratch,
        compiler_params=pltpu.CompilerParams(
            collective_id=0, has_side_effects=True, vmem_limit_bytes=60 * 1024 * 1024
        ),
    )(*args)
    return pl.pallas_call(
        hand_over,
        out_shape=shapes,
        in_specs=[pl.BlockSpec(memory_space=pltpu.VMEM)] * 4,
        out_specs=[pl.BlockSpec(memory_space=pltpu.VMEM)] * 3,
    )(*made)


def solution(mesh):
    placed = (
        P(("grp", "ep"), None),
        P(("grp", "ep"), None, "tp"),
        P(("grp", "ep"), "tp"),
        P(),
        P(),
        P("ep", "tp"),
        P("ep", "tp"),
        P(None, "tp"),
        P("tp", None, None),
        P("tp", None, None),
        P("tp"),
        P("tp", None),
        P("grp", None),
        P("grp", None),
        P("ep", None, "tp"),
        P("ep", None, "tp"),
        P("ep", "tp", None),
        P(),
        P(None, ("ep", "tp")),
        P(None, ("ep", "tp")),
        P(("ep", "tp"), None),
    )
    return jax.shard_map(
        functools.partial(on_device, mesh.shape["ep"], mesh.shape["tp"]),
        mesh=mesh,
        in_specs=placed,
        out_specs=(P(("grp", "ep"), "tp"), P(("grp", "ep"), "tp"), P(("grp", "ep"), None, "tp")),
        check_vma=False,
    )
```
